32 devices in a mesh: sp: 8 (over z, core), tp: 4 (over y, x).
Axes of the slice: x: 2, y: 2, z: 4, core: 2. Of those that a mesh axis runs over, the one named last changes fastest.
Arguments:
- resid: bfloat16 [2048, 2048], P('sp'), may hold values from -18 to 18
- narrow_head_input: bfloat16 [2048, 1024], P('sp', 'tp'), may hold values from -6 to 6
- wide_head_input: bfloat16 [2048, 2048], P('sp', 'tp'), may hold values from -6 to 6
- key_group_input: bfloat16 [2048, 512], P('sp'), may hold values from -6 to 6
- query_group_input: bfloat16 [2048, 512], P('sp'), may hold values from -6 to 6
- narrow_output_gate: bfloat16 [2048, 1024], P('sp', 'tp'), may hold values from -6 to 6
- wide_output_gate: bfloat16 [2048, 2048], P('sp', 'tp'), may hold values from -6 to 6
- step_input_rows: bfloat16 [2048, 2, 16], P('sp', None, 'tp'), may hold values from -4 to 4
- head_decay_logarithm: float32 [2, 16], P(None, 'tp'), may hold values from -14 to -2
- position_log_decay: float32 [2048, 2, 16], P('sp', None, 'tp'), may hold values from -1.4 to 0
- direct_input_weight: float32 [2, 16], P(None, 'tp'), may hold values from 0.5 to 2
- narrow_conv_taps: float32 [4, 1024], P(None, 'tp'), may hold values from -3 to 3
- wide_conv_taps: float32 [4, 2048], P(None, 'tp'), may hold values from -3 to 3
- key_conv_taps: float32 [4, 512], replicated, may hold values from -3 to 3
- query_conv_taps: float32 [4, 512], replicated, may hold values from -3 to 3
- narrow_norm_gain: float32 [1024], P('tp'), may hold values from 0.1 to 1.9
- wide_norm_gain: float32 [2048], P('tp'), may hold values from 0.1 to 1.9
- narrow_output_rows: bfloat16 [1024, 2048], P('tp'), may hold values from -0.109375 to 0.109375
- wide_output_rows: bfloat16 [2048, 2048], P('tp'), may hold values from -0.109375 to 0.109375
- feedforward_norm_gain: float32 [2048], replicated, may hold values from 0.1 to 1.9
- routes: int32 [2048, 3], P('sp'), may hold values from 0 to 7, all different within a row; in each aligned block of 256 rows (0 to 255, 256 to 511, ...) at most 128 rows name the same one
- routing_weight_values: float32 [2048, 3], P('sp'), may hold values from 0.1 to 1
- expert_gate_matrix: bfloat16 [8, 2048, 2048], P('sp', None, 'tp'), may hold values from -1 to 1
- expert_up_matrix: bfloat16 [8, 2048, 2048], P('sp', None, 'tp'), may hold values from -1 to 1
- expert_down_matrix: bfloat16 [8, 2048, 2048], P('sp', 'tp'), may hold values from -0.015625 to 0.015625
Outputs:
- layer_out: bfloat16 [2048, 2048], P('sp', 'tp')
The draws below stay inside these ranges and needn't reach their ends.
Inputs may be any that keep to these rules, and one draw needn't show every extreme that they name: `routes`: each token names 3 different experts. Among the tokens of one index of sp (aligned blocks of 256 rows) no expert is named by more than 128 of them, and in some blocks one is named by exactly 128.
All inputs are finite; a program needn't handle non-finite values.
Results may differ from the reference program's by a relative error of at most 0.015.
Values may be sent and summed in bfloat16 or wider, within the bound.
A program may use at most 64 MiB of HBM per device.

```python
import math
import jax
import jax.numpy as jnp
import numpy as np
from jax import lax

D = 2048
HEADS = 16
NARROW_HEAD_DIM = 64
WIDE_HEAD_DIM = 128
STATE = 128
GROUPS = 4
CONV_W = 4
BLOCK = 128
FF = 2048
TOPK = 3
TOK_SP = 256
TOKENS = 2048
EXPERTS = 8
CAP = 128
N_SP = 8
N_TP = 4


def draw_resid(key, part):
    key_base, key_rows = jax.random.split(jax.random.fold_in(key, 3), 2)
    row_scales = jnp.exp(jax.random.uniform(key_rows, (TOKENS, 1), jnp.float32, math.log(0.3), math.log(3.0)))
    base = jnp.clip(jax.random.normal(key_base, (TOKENS, D), jnp.float32), -6.0, 6.0)
    return jnp.clip(base * row_scales, -18.0, 18.0).astype(jnp.bfloat16)


def draw_step_input_rows(key, part):
    key_base, key_shift = jax.random.split(jax.random.fold_in(key, 5))
    block_total = TOKENS // TOK_SP
    shifts = jax.random.uniform(key_shift, (block_total, 1, 1, 1), jnp.float32, -1.0, 1.0)
    base = jax.random.normal(key_base, (block_total, TOK_SP, 2, HEADS), jnp.float32)
    return jnp.clip(base + shifts, -4.0, 4.0).reshape(TOKENS, 2, HEADS).astype(jnp.bfloat16)


def draw_head_decay_logarithm(key, part):
    key_kind, key_slow, key_fast = jax.random.split(jax.random.fold_in(key, 7), 3)
    slow_share = 0.5
    slow_heads = jax.random.uniform(key_kind, (2, HEADS), jnp.float32) < slow_share
    slow_rate = jnp.exp(jax.random.uniform(key_slow, (2, HEADS), jnp.float32, math.log(0.1), math.log(0.6))) / TOKENS
    fast_rate = jnp.exp(jax.random.uniform(key_fast, (2, HEADS), jnp.float32, math.log(1.0 / 60.0), math.log(1.0 / 20.0)))
    return jnp.clip(jnp.log(jnp.where(slow_heads, slow_rate, fast_rate)), -14.0, -2.0).astype(jnp.float32)


def draw_position_log_decay(key, part):
    key_spots, key_depth = jax.random.split(jax.random.fold_in(key, 9))
    spots = jax.random.randint(key_spots, (3,), 0, TOKENS)
    depth = jax.random.uniform(key_depth, (3, 2, HEADS), jnp.float32, math.log(0.5), math.log(0.8))
    hits = (jnp.arange(TOKENS)[:, None] == spots[None, :]).astype(jnp.float32)
    return jnp.clip(jnp.einsum('tk,khd->thd', hits, depth), -1.4, 0.0).astype(jnp.float32)


def draw_expert_gate_matrix(key, part):
    key_base, key_cols = jax.random.split(jax.random.fold_in(key, 11))
    column_scales = jnp.exp(jax.random.uniform(key_cols, (EXPERTS, 1, FF), jnp.float32, math.log(0.5), math.log(8.0)))
    base = jax.random.normal(key_base, (EXPERTS, D, FF), jnp.float32)
    return jnp.clip(base * column_scales / math.sqrt(D), -1.0, 1.0).astype(jnp.bfloat16)


def draw_expert_up_matrix(key, part):
    key_base, key_cols = jax.random.split(jax.random.fold_in(key, 13))
    column_scales = jnp.exp(jax.random.uniform(key_cols, (EXPERTS, 1, FF), jnp.float32, math.log(0.5), math.log(8.0)))
    base = jax.random.normal(key_base, (EXPERTS, D, FF), jnp.float32)
    return jnp.clip(base * column_scales / math.sqrt(D), -1.0, 1.0).astype(jnp.bfloat16)


def level_of(own_key, dims, shards, least, high):
    def one(dim, blocks):
        draws = jax.random.uniform(jax.random.fold_in(jax.random.fold_in(own_key, 6), dim), (blocks,), jnp.float32, least / len(shards), high / len(shards))
        return jnp.repeat(jnp.exp(draws), dims[dim] // blocks).reshape((-1,) + (1,) * (len(dims) - dim - 1))

    gain = one(*shards[0])
    for cut in shards[1:]:
        gain = gain * one(*cut)
    return gain


def shared_out(rng, own, number, rows, amount, top, limit, lean):
    sequence = jax.random.permutation(rng, amount)
    crowded, common = portions_of(amount, rows * top, limit, lean, True), portions_of(amount, rows * top, limit, lean, False)
    places = jnp.arange(amount)

    def named(tallies, offset_by):
        used = int((tallies > 0).sum())
        fixed = max(1, used // 4)
        moved = fixed + (places - fixed + offset_by * (used - fixed)) % max(1, amount - fixed)
        return jnp.zeros((amount,), jnp.int32).at[sequence[jnp.where(places < fixed, places, moved)]].set(jnp.asarray(tallies, jnp.int32))

    tallies = jnp.where(number % 4 == 0, named(crowded, number // 4), named(common, number - number // 4 - 1))
    mixed = jax.random.permutation(jax.random.fold_in(own, 3), amount)
    giver, sink = mixed[0:amount // 2 * 2:2], mixed[1:amount // 2 * 2:2]
    margin = jnp.minimum(tallies[giver] - 1, limit - tallies[sink]) // 2
    margin = jnp.where((giver == sequence[0]) | (sink == sequence[0]) | (tallies[sink] == 0), 0, jnp.maximum(margin, 0))
    moved = jax.random.randint(jax.random.fold_in(own, 4), (amount // 2,), 0, 1 << 20) % (margin + 1)
    tallies = tallies.at[giver].add(-moved).at[sink].add(moved)
    members = jnp.searchsorted(jnp.cumsum(tallies), jnp.arange(rows * top), side="right").astype(jnp.int32)
    listing = members.reshape(top, rows).T
    listing = listing[jax.random.permutation(jax.random.fold_in(own, 1), rows)]
    offset_by = jax.random.randint(jax.random.fold_in(own, 2), (rows, 1), 0, top)
    return jnp.take_along_axis(listing, (jnp.arange(top)[None, :] + offset_by) % top, axis=1)


def portions_of(number_of, total, bound, lean, full):
    portions = [(1 << 20) // math.isqrt(standing ** lean) + 1 for standing in range(1, number_of + 1)]
    largest = bound if full else min(bound, max(-(-total // number_of), total * portions[0] // sum(portions)))
    least = 1 if total - largest >= number_of - 1 else 0
    holding, surplus = [largest] + [least] * (number_of - 1), total - largest - least * (number_of - 1)
    while surplus > 0:
        movable = [i for i in range(1, number_of) if holding[i] < largest] or [i for i in range(1, number_of) if holding[i] < bound]
        pool, left = sum([portions[i] for i in movable]), surplus
        for i in movable:
            extra = min(bound - holding[i], max(1, left * portions[i] // pool), surplus)
            holding[i] = holding[i] + extra
            surplus = surplus - extra
    return np.array(holding)


def normal_values(rng, shape, deviation, limit, cuts=(), kind=jnp.bfloat16):
    drawn = deviation * jax.random.normal(rng, shape, jnp.float32)
    if cuts:
        drawn = drawn * level_of(rng, shape, cuts, -0.22, 0.18)
    return jnp.clip(drawn, -limit, limit).astype(kind)


def setup_inputs(seed: int = 0) -> dict:
    splits = jax.random.split(jax.random.key(seed), 26)
    resid = draw_resid(jax.random.fold_in(splits[25], 71), 0)
    narrow_head_input = normal_values(splits[1], (TOKENS, HEADS * NARROW_HEAD_DIM), 1.0, 6.0, ((0, 8), (1, 4)))
    wide_head_input = normal_values(splits[2], (TOKENS, HEADS * WIDE_HEAD_DIM), 1.0, 6.0, ((0, 8), (1, 4)))
    key_group_input = normal_values(splits[3], (TOKENS, GROUPS * STATE), 1.0, 6.0, ((0, 8),))
    query_group_input = normal_values(splits[4], (TOKENS, GROUPS * STATE), 1.0, 6.0, ((0, 8),))
    narrow_output_gate = normal_values(splits[5], (TOKENS, HEADS * NARROW_HEAD_DIM), 1.0, 6.0, ((0, 8), (1, 4)))
    wide_output_gate = normal_values(splits[6], (TOKENS, HEADS * WIDE_HEAD_DIM), 1.0, 6.0, ((0, 8), (1, 4)))
    step_input_rows = draw_step_input_rows(jax.random.fold_in(splits[25], 71), 0)
    head_decay_logarithm = draw_head_decay_logarithm(jax.random.fold_in(splits[25], 71), 0)
    position_log_decay = draw_position_log_decay(jax.random.fold_in(splits[25], 71), 0)
    direct_input_weight = jnp.clip(0.5 + 1.5 * jax.random.uniform(splits[10], (2, HEADS), jnp.float32) ** level_of(splits[10], (2, HEADS), ((1, 4),), -0.2, 0.2), 0.5, 2.0)
    narrow_conv_taps = normal_values(splits[11], (CONV_W, HEADS * NARROW_HEAD_DIM), CONV_W ** -0.5, 3.0, ((1, 4),), jnp.float32)
    wide_conv_taps = normal_values(splits[12], (CONV_W, HEADS * WIDE_HEAD_DIM), CONV_W ** -0.5, 3.0, ((1, 4),), jnp.float32)
    key_conv_taps = normal_values(splits[13], (CONV_W, GROUPS * STATE), CONV_W ** -0.5, 3.0, (), jnp.float32)
    query_conv_taps = normal_values(splits[14], (CONV_W, GROUPS * STATE), CONV_W ** -0.5, 3.0, (), jnp.float32)
    narrow_norm_gain = jnp.clip(1.0 + 0.18 * jax.random.normal(splits[15], (HEADS * NARROW_HEAD_DIM,), jnp.float32), 0.1, 1.9)
    wide_norm_gain = jnp.clip(1.0 + 0.18 * jax.random.normal(splits[16], (HEADS * WIDE_HEAD_DIM,), jnp.float32), 0.1, 1.9)
    narrow_output_rows = normal_values(splits[17], (HEADS * NARROW_HEAD_DIM, D), (HEADS * (NARROW_HEAD_DIM + WIDE_HEAD_DIM)) ** -0.5, 0.109375, ((0, 4),))
    wide_output_rows = normal_values(splits[18], (HEADS * WIDE_HEAD_DIM, D), (HEADS * (NARROW_HEAD_DIM + WIDE_HEAD_DIM)) ** -0.5, 0.109375, ((0, 4),))
    feedforward_norm_gain = jnp.clip(1.0 + 0.18 * jax.random.normal(splits[19], (D,), jnp.float32), 0.1, 1.9)
    routes_keys = jax.random.split(jax.random.fold_in(splits[20], 1), TOKENS // TOK_SP)
    routes_turns = jax.random.permutation(jax.random.fold_in(splits[20], 3), TOKENS // TOK_SP)
    routes = jax.vmap(lambda own, number: shared_out(jax.random.fold_in(splits[20], 2), own, number, TOK_SP, EXPERTS, TOPK, CAP, 1))(routes_keys, routes_turns).reshape((TOKENS, TOPK))
    routing_weight_values = jnp.clip(0.1 + 0.9 * jax.random.uniform(splits[21], (TOKENS, TOPK), jnp.float32) ** level_of(splits[21], (TOKENS, TOPK), ((0, 8),), -0.2, 0.2), 0.1, 1.0)
    expert_gate_matrix = draw_expert_gate_matrix(jax.random.fold_in(splits[25], 71), 0)
    expert_up_matrix = draw_expert_up_matrix(jax.random.fold_in(splits[25], 71), 0)
    expert_down_matrix = normal_values(splits[24], (EXPERTS, FF, D), (64 * FF) ** -0.5, 0.015625, ((0, 8), (1, 4)))
    return {"resid": resid, "narrow_head_input": narrow_head_input, "wide_head_input": wide_head_input, "key_group_input": key_group_input, "query_group_input": query_group_input, "narrow_output_gate": narrow_output_gate, "wide_output_gate": wide_output_gate, "step_input_rows": step_input_rows, "head_decay_logarithm": head_decay_logarithm, "position_log_decay": position_log_decay, "direct_input_weight": direct_input_weight, "narrow_conv_taps": narrow_conv_taps, "wide_conv_taps": wide_conv_taps, "key_conv_taps": key_conv_taps, "query_conv_taps": query_conv_taps, "narrow_norm_gain": narrow_norm_gain, "wide_norm_gain": wide_norm_gain, "narrow_output_rows": narrow_output_rows, "wide_output_rows": wide_output_rows, "feedforward_norm_gain": feedforward_norm_gain, "routes": routes, "routing_weight_values": routing_weight_values, "expert_gate_matrix": expert_gate_matrix, "expert_up_matrix": expert_up_matrix, "expert_down_matrix": expert_down_matrix}


NORM_EPS = 1e-06
CLAMP_LIMIT = 7.0
SIGMOID_SCALE = 1.702
FULL_PRECISION = lax.Precision.HIGHEST

def conv_with_rim(values, rim_rows, weight):
    length = values.shape[0]
    padded = jnp.concatenate([rim_rows, values], axis=0).astype(jnp.float32)
    accumulated = jnp.zeros((length, values.shape[1]), jnp.float32)
    for tap_index in range(weight.shape[0]):
        accumulated = accumulated + weight[tap_index] * padded[tap_index:tap_index + length]
    return jax.nn.silu(accumulated)

def pick_groups(channel_table, first_head, head_count):
    length = channel_table.shape[0]
    grouped = channel_table.reshape(length, GROUPS, -1)
    owners = (first_head + jnp.arange(head_count, dtype=jnp.int32)) // (HEADS // GROUPS)
    chooser = (owners[:, None] == jnp.arange(GROUPS, dtype=jnp.int32)[None, :]).astype(jnp.float32)
    return jnp.einsum('sgn,hg->shn', grouped, chooser, precision=FULL_PRECISION)

def local_head(values, step_logarithm, key_head_rows, query_head_rows, block_len):
    block_count = values.shape[0] // block_len
    values = values.reshape(block_count, block_len, -1)
    step_logarithm = step_logarithm.reshape(block_count, block_len)
    key_head_rows = key_head_rows.reshape(block_count, block_len, -1)
    query_head_rows = query_head_rows.reshape(block_count, block_len, -1)
    cum_decay = jnp.cumsum(step_logarithm, axis=1)
    causal_mask = jnp.arange(block_len)[:, None] >= jnp.arange(block_len)[None, :]
    decay_gaps = jnp.where(causal_mask[None], cum_decay[:, :, None] - cum_decay[:, None, :], -1e+30)
    scores = jnp.einsum('bln,bsn->bls', query_head_rows, key_head_rows, precision=FULL_PRECISION) * jnp.exp(decay_gaps)
    inside = jnp.einsum('bls,bsp->blp', scores, values, precision=FULL_PRECISION)
    tail_decay = jnp.exp(cum_decay[:, -1:] - cum_decay)
    states = jnp.einsum('bln,blp->bnp', key_head_rows * tail_decay[..., None], values, precision=FULL_PRECISION)
    totals = cum_decay[:, -1]

    def walk(running, member):
        return (jnp.exp(member[1]) * running + member[0], running)
    closing, entering = lax.scan(walk, jnp.zeros(states.shape[1:], jnp.float32), (states, totals))
    before = jnp.cumsum(totals) - totals
    return (inside, entering, closing, jnp.sum(totals), before, cum_decay, query_head_rows)

def finish_head(inside, entering, before, cum_decay, query_blocks, carried):
    starting = entering + jnp.exp(before)[:, None, None] * carried[None]
    readout = jnp.einsum('bln,bnp->blp', query_blocks * jnp.exp(cum_decay)[..., None], starting, precision=FULL_PRECISION)
    return (inside + readout).reshape(-1, inside.shape[-1])

def group_out(scanned, mixed_input_rows, direct_input_term, gate_input_rows, norm_gain_vector):
    length, head_count, head_dimension = mixed_input_rows.shape
    gated = jax.nn.silu(gate_input_rows.astype(jnp.float32)).reshape(length, head_count, head_dimension)
    result = (scanned + direct_input_term[None, :, None] * mixed_input_rows) * gated
    result = result * lax.rsqrt(lax.optimization_barrier(jnp.mean(result * result, axis=-1, keepdims=True)) + NORM_EPS)
    return (result.reshape(length, head_count * head_dimension) * norm_gain_vector).astype(jnp.bfloat16)

def mixer_head_group(unprojected_input, gate_input_rows, convolution_weight, key_head_table, query_head_table, unsoftened_step, decay_vector, position_decay_rows, direct_input_term, norm_gain_vector, head_dimension):
    length = unprojected_input.shape[0]
    zero_rim = jnp.zeros((convolution_weight.shape[0] - 1, unprojected_input.shape[1]), unprojected_input.dtype)
    mixed_input_rows = conv_with_rim(unprojected_input, zero_rim, convolution_weight).reshape(length, -1, head_dimension)
    head_count = mixed_input_rows.shape[1]
    key_head_rows = pick_groups(key_head_table, 0, head_count)
    query_head_rows = pick_groups(query_head_table, 0, head_count)
    step_length_values = jax.nn.softplus(unsoftened_step.astype(jnp.float32))
    step_logarithm = -jnp.exp(decay_vector)[None, :] * step_length_values + position_decay_rows
    values = mixed_input_rows * step_length_values[..., None]

    def one_head(head_values, head_log, head_keys, head_queries):
        parts = local_head(head_values, head_log, head_keys, head_queries, BLOCK)
        return finish_head(parts[0], parts[1], parts[4], parts[5], parts[6], jnp.zeros_like(parts[2]))
    scanned = jax.vmap(one_head, in_axes=(1, 1, 1, 1), out_axes=1)(values, step_logarithm, key_head_rows, query_head_rows)
    return group_out(scanned, mixed_input_rows, direct_input_term, gate_input_rows, norm_gain_vector)

def expert_layer(normed, routes, expert_gate_matrix, expert_up_matrix, expert_down_matrix):
    tokens = normed.shape[0]
    flat_routes = routes.reshape(-1).astype(jnp.int32)
    order_ids = jnp.argsort(flat_routes, stable=True).astype(jnp.int32)
    sorted_routes = flat_routes[order_ids]
    counts = lax.optimization_barrier(jnp.sum((flat_routes[:, None] == jnp.arange(EXPERTS, dtype=jnp.int32)[None, :]).astype(jnp.int32), axis=0))
    starts = (jnp.cumsum(counts) - counts).astype(jnp.int32)
    room = CAP * N_SP
    padded_ids = jnp.concatenate([order_ids, jnp.zeros((room,), jnp.int32)])

    def one_expert(member):
        start, gate_weight, up_weight, down_weight = member
        picked = lax.dynamic_slice_in_dim(padded_ids, start, room)
        rows = normed[picked // TOPK]
        gate_pre = jnp.dot(rows, gate_weight, preferred_element_type=jnp.float32)
        up_pre = jnp.dot(rows, up_weight, preferred_element_type=jnp.float32)
        clamped = jnp.minimum(gate_pre, CLAMP_LIMIT)
        act = ((jnp.clip(up_pre, -CLAMP_LIMIT, CLAMP_LIMIT) + 1.0) * clamped * jax.nn.sigmoid(SIGMOID_SCALE * clamped)).astype(jnp.bfloat16)
        pieces = act.reshape(room, N_TP, -1).astype(jnp.float32)
        blocks = down_weight.reshape(N_TP, -1, down_weight.shape[1]).astype(jnp.float32)
        partials = jnp.einsum('rtf,tfd->rtd', pieces, blocks)
        rounded = lax.optimization_barrier(partials.astype(jnp.bfloat16)).astype(jnp.float32)
        return lax.optimization_barrier(jnp.sum(rounded, axis=1)).astype(jnp.bfloat16)
    outputs = lax.map(one_expert, (starts, expert_gate_matrix, expert_up_matrix, expert_down_matrix))
    within = jnp.arange(tokens * TOPK, dtype=jnp.int32) - starts[sorted_routes]
    per_sorted = outputs.reshape(EXPERTS * room, -1)[sorted_routes * room + within]
    per_entry = jnp.zeros((tokens * TOPK, per_sorted.shape[1]), jnp.bfloat16).at[order_ids].set(per_sorted)
    return per_entry.reshape(tokens, TOPK, -1)

def reference(resid, narrow_head_input, wide_head_input, key_group_input, query_group_input, narrow_output_gate, wide_output_gate, step_input_rows, head_decay_logarithm, position_log_decay, direct_input_weight, narrow_conv_taps, wide_conv_taps, key_conv_taps, query_conv_taps, narrow_norm_gain, wide_norm_gain, narrow_output_rows, wide_output_rows, feedforward_norm_gain, routes, routing_weight_values, expert_gate_matrix, expert_up_matrix, expert_down_matrix):
    length = resid.shape[0]
    zero_rim = jnp.zeros((CONV_W - 1, key_group_input.shape[1]), key_group_input.dtype)
    key_head_table = conv_with_rim(key_group_input, zero_rim, key_conv_taps)
    query_head_table = conv_with_rim(query_group_input, zero_rim, query_conv_taps)
    narrow_head_output = mixer_head_group(narrow_head_input, narrow_output_gate, narrow_conv_taps, key_head_table, query_head_table, step_input_rows[:, 0], head_decay_logarithm[0], position_log_decay[:, 0], direct_input_weight[0], narrow_norm_gain, NARROW_HEAD_DIM)
    wide_head_output = mixer_head_group(wide_head_input, wide_output_gate, wide_conv_taps, key_head_table, query_head_table, step_input_rows[:, 1], head_decay_logarithm[1], position_log_decay[:, 1], direct_input_weight[1], wide_norm_gain, WIDE_HEAD_DIM)
    narrow_blocks = narrow_head_output.reshape(length, N_TP, -1).transpose(1, 0, 2)
    wide_blocks = wide_head_output.reshape(length, N_TP, -1).transpose(1, 0, 2)
    narrow_weights = narrow_output_rows.reshape(N_TP, -1, narrow_output_rows.shape[1])
    wide_weights = wide_output_rows.reshape(N_TP, -1, wide_output_rows.shape[1])

    def project(running, member):
        part_narrow, part_wide, weight_narrow, weight_wide = member
        term = jnp.dot(part_narrow, weight_narrow, preferred_element_type=jnp.float32)
        term = term + jnp.dot(part_wide, weight_wide, preferred_element_type=jnp.float32)
        return (running + lax.optimization_barrier(term.astype(jnp.bfloat16)).astype(jnp.float32), None)
    mixed, _ = lax.scan(project, jnp.zeros((length, narrow_output_rows.shape[1]), jnp.float32), (narrow_blocks, wide_blocks, narrow_weights, wide_weights))
    hidden_state = resid.astype(jnp.float32) + mixed
    normed = (hidden_state * lax.rsqrt(lax.optimization_barrier(jnp.mean(hidden_state * hidden_state, axis=-1, keepdims=True)) + NORM_EPS) * feedforward_norm_gain).astype(jnp.bfloat16)
    expert_rows = expert_layer(normed, routes, expert_gate_matrix, expert_up_matrix, expert_down_matrix)
    combined = lax.optimization_barrier(jnp.sum(expert_rows.astype(jnp.float32) * routing_weight_values[..., None], axis=1))
    return (hidden_state + combined).astype(jnp.bfloat16)
```

```python
import functools

import jax
import jax.numpy as jnp
from jax import lax
from jax.experimental import pallas as pl
from jax.experimental.pallas import tpu as pltpu
from jax.sharding import PartitionSpec as P

HEADS = 16
NARROW_HEAD_DIM = 64
WIDE_HEAD_DIM = 128
GROUPS = 4
BLOCK = 128


NORM_EPS = 1e-06
CLAMP_LIMIT = 7.0
SIGMOID_SCALE = 1.702
FULL_PRECISION = lax.Precision.HIGHEST


def passed_along(block, axis, distance):
    devices = range(lax.axis_size(axis))
    route = [(i - distance, i) for i in devices if i - distance in devices]
    return lax.ppermute(block, axis, route)


def entering_2(x, axis, join, neutral):
    place = lax.axis_index(axis)
    gathered = jax.tree.map(
        lambda a, kind: lax.all_gather(a.astype(kind), axis),
        x,
        jax.tree.map(lambda a: jnp.bfloat16 if a.dtype == jnp.float32 else a.dtype, x),
    )
    state = jax.tree.map(lambda a, e: jnp.zeros_like(a) + jnp.asarray(e, a.dtype), x, neutral)

    def one(lap, state):
        return join(
            state,
            jax.tree.map(
                lambda a, own: lax.dynamic_index_in_dim(a, lap, 0, False).astype(own.dtype),
                gathered,
                x,
            ),
        )

    return lax.fori_loop(0, place, one, state)


def conv_with_rim(values, rim_rows, weight):
    length = values.shape[0]
    padded = jnp.concatenate([rim_rows, values], axis=0).astype(jnp.float32)
    accumulated = jnp.zeros((length, values.shape[1]), jnp.float32)
    for tap_index in range(weight.shape[0]):
        accumulated = accumulated + weight[tap_index] * padded[tap_index : tap_index + length]
    return jax.nn.silu(accumulated)


def pick_groups(channel_table, first_head, head_count):
    length = channel_table.shape[0]
    grouped = channel_table.reshape(length, GROUPS, -1)
    owners = (first_head + jnp.arange(head_count, dtype=jnp.int32)) // (HEADS // GROUPS)
    chooser = (owners[:, None] == jnp.arange(GROUPS, dtype=jnp.int32)[None, :]).astype(jnp.float32)
    return jnp.einsum("sgn,hg->shn", grouped, chooser, precision=FULL_PRECISION)


def local_head(values, step_logarithm, key_head_rows, query_head_rows, block_len):
    block_count = values.shape[0] // block_len
    values = values.reshape(block_count, block_len, -1)
    step_logarithm = step_logarithm.reshape(block_count, block_len)
    key_head_rows = key_head_rows.reshape(block_count, block_len, -1)
    query_head_rows = query_head_rows.reshape(block_count, block_len, -1)
    cum_decay = jnp.cumsum(step_logarithm, axis=1)
    causal_mask = jnp.arange(block_len)[:, None] >= jnp.arange(block_len)[None, :]
    decay_gaps = jnp.where(causal_mask[None], cum_decay[:, :, None] - cum_decay[:, None, :], -1e30)
    scores = jnp.einsum(
        "bln,bsn->bls", query_head_rows, key_head_rows, precision=FULL_PRECISION
    ) * jnp.exp(decay_gaps)
    inside = jnp.einsum("bls,bsp->blp", scores, values, precision=FULL_PRECISION)
    tail_decay = jnp.exp(cum_decay[:, -1:] - cum_decay)
    states = jnp.einsum(
        "bln,blp->bnp", key_head_rows * tail_decay[..., None], values, precision=FULL_PRECISION
    )
    totals = cum_decay[:, -1]

    def walk(running, member):
        return (jnp.exp(member[1]) * running + member[0], running)

    closing, entering = lax.scan(walk, jnp.zeros(states.shape[1:], jnp.float32), (states, totals))
    before = jnp.cumsum(totals) - totals
    return (inside, entering, closing, jnp.sum(totals), before, cum_decay, query_head_rows)


def finish_head(inside, entering, before, cum_decay, query_blocks, carried):
    starting = entering + jnp.exp(before)[:, None, None] * carried[None]
    readout = jnp.einsum(
        "bln,bnp->blp",
        query_blocks * jnp.exp(cum_decay)[..., None],
        starting,
        precision=FULL_PRECISION,
    )
    return (inside + readout).reshape(-1, inside.shape[-1])


def group_out(scanned, mixed_input_rows, direct_input_term, gate_input_rows, norm_gain_vector):
    length, head_count, head_dimension = mixed_input_rows.shape
    gated = jax.nn.silu(gate_input_rows.astype(jnp.float32)).reshape(
        length, head_count, head_dimension
    )
    result = (scanned + direct_input_term[None, :, None] * mixed_input_rows) * gated
    result = result * lax.rsqrt(jnp.mean(result * result, axis=-1, keepdims=True) + NORM_EPS)
    return (result.reshape(length, head_count * head_dimension) * norm_gain_vector).astype(
        jnp.bfloat16
    )


def head_pieces_list(
    mixed_input_rows,
    step_length_values,
    decay_vector,
    position_decay_rows,
    key_head_rows,
    query_head_rows,
):
    step_logarithm = -jnp.exp(decay_vector)[None, :] * step_length_values + position_decay_rows
    values = mixed_input_rows * step_length_values[..., None]
    walker = functools.partial(local_head, block_len=BLOCK)
    return jax.vmap(walker, in_axes=(1, 1, 1, 1))(
        values, step_logarithm, key_head_rows, query_head_rows
    )


def finish_group(parts, carried_states):
    return jax.vmap(finish_head, in_axes=(0, 0, 0, 0, 0, 0), out_axes=1)(
        parts[0], parts[1], parts[4], parts[5], parts[6], carried_states
    )


def chain_combine(earlier, later):
    return (
        earlier[0] + later[0],
        earlier[1] + later[1],
        jnp.exp(later[0])[:, None, None] * earlier[2] + later[2],
        jnp.exp(later[1])[:, None, None] * earlier[3] + later[3],
    )


def ring_map(index, count):
    side = int(round(count**0.5))
    if side * side != count:
        return index
    row = index // side
    column = index % side
    return row * side + column + (row % 2) * (side - 1 - 2 * column)


def tail_kernel(
    shards,
    experts,
    narrow_ref,
    wide_ref,
    narrow_rows_ref,
    wide_rows_ref,
    resid_ref,
    gain_ref,
    rank_ref,
    weight_ref,
    gate_hbm,
    up_hbm,
    down_hbm,
    out_ref,
    gate_v,
    up_v,
    down_v,
    share_out,
    share_in,
    square_out,
    square_in,
    hidden,
    normed,
    dispatch_out,
    tokens,
    partial,
    sums,
    done_out,
    done_in,
    load_sem,
    share_send,
    share_recv,
    square_send,
    square_recv,
    dispatch_send,
    dispatch_recv,
    gather_send,
    gather_recv,
    sum_send,
    sum_recv,
    done_send,
    done_recv,
):
    me_s = lax.axis_index("sp")
    me_t = lax.axis_index("tp")
    length, width = resid_ref.shape
    capacity = done_in.shape[1]
    groups = tokens.shape[1]
    sources = experts // groups
    half = tokens.shape[2] // 2
    place = ring_map(me_t, shards)
    after = ring_map((place + 1) % shards, shards)
    before = ring_map((place + shards - 1) % shards, shards)

    def remote(src, dst, send, recv, where):
        return pltpu.make_async_remote_copy(
            src_ref=src,
            dst_ref=dst,
            send_sem=send,
            recv_sem=recv,
            device_id=where,
            device_id_type=pl.DeviceIdType.MESH,
        )

    loads = [
        pltpu.make_async_copy(h, v, load_sem.at[i])
        for i, (h, v) in enumerate(((gate_hbm, gate_v), (up_hbm, up_v), (down_hbm, down_v)))
    ]
    for load in loads:
        load.start()

    barrier = pltpu.get_barrier_semaphore()

    def greet_tp(d, c):
        pl.semaphore_signal(
            barrier,
            inc=1,
            device_id=(me_s, (me_t + d) % shards),
            device_id_type=pl.DeviceIdType.MESH,
        )
        return c

    def greet_sp(d, c):
        pl.semaphore_signal(
            barrier,
            inc=1,
            device_id=((me_s + d) % experts, me_t),
            device_id_type=pl.DeviceIdType.MESH,
        )
        return c

    lax.fori_loop(1, shards, greet_tp, 0)
    lax.fori_loop(1, experts, greet_sp, 0)
    pl.semaphore_wait(barrier, shards + experts - 2)

    def project(block):
        columns = pl.ds(pl.multiple_of(block * width, 128), width)
        return (
            jnp.dot(
                narrow_ref[...], narrow_rows_ref[:, columns], preferred_element_type=jnp.float32
            )
            + jnp.dot(wide_ref[...], wide_rows_ref[:, columns], preferred_element_type=jnp.float32)
        ).astype(jnp.bfloat16)

    def share_copy(d):
        return remote(
            share_out.at[d],
            share_in.at[d],
            share_send.at[d],
            share_recv.at[d],
            (me_s, (me_t + d) % shards),
        )

    def send_share(d, c):
        share_out[d] = project((me_t + d) % shards)
        share_copy(d).start()
        return c

    lax.fori_loop(1, shards, send_share, 0)
    hidden[...] = resid_ref[...].astype(jnp.float32) + project(me_t).astype(jnp.float32)

    def take_share(d, c):
        share_copy(d).wait_recv()
        hidden[...] += share_in[d].astype(jnp.float32)
        return c

    lax.fori_loop(1, shards, take_share, 0)
    state = hidden[...]
    own_square = jnp.sum(state * state, axis=1, keepdims=True)
    square_rows = jnp.transpose(jnp.broadcast_to(own_square, (length, 128)))
    square_out[...] = square_rows[:8]

    def square_copy(d):
        return remote(
            square_out,
            square_in.at[d],
            square_send.at[d],
            square_recv.at[d],
            (me_s, (me_t + d) % shards),
        )

    def send_square(d, c):
        square_copy(d).start()
        return c

    lax.fori_loop(1, shards, send_square, 0)

    def take_square(d, total):
        square_copy(d).wait_recv()
        return total + square_in[d]

    total = lax.fori_loop(1, shards, take_square, square_rows[:8])
    scale_row = lax.rsqrt(total[:1] / (shards * width) + NORM_EPS)
    scale = jnp.transpose(jnp.broadcast_to(scale_row, (128, length)))[:, :1]
    normed[...] = (hidden[...] * scale * gain_ref[...]).astype(jnp.bfloat16)

    slots = lax.broadcasted_iota(jnp.int32, (capacity, length), 0)

    def pick(d):
        chooser = jnp.where(slots == rank_ref[d], 1.0, 0.0).astype(jnp.bfloat16)
        return jnp.dot(chooser, normed[...], preferred_element_type=jnp.float32).astype(
            jnp.bfloat16
        )

    def dispatch_copy(d):
        return remote(
            dispatch_out.at[d],
            tokens.at[me_t, d // sources, pl.ds((d % sources) * capacity, capacity)],
            dispatch_send.at[d],
            dispatch_recv.at[d],
            ((me_s + d) % experts, me_t),
        )

    def send_dispatch(d, c):
        dispatch_out[d] = pick(d)
        dispatch_copy(d).start()
        return c

    tokens[me_t, 0, :capacity] = pick(0)
    lax.fori_loop(1, experts, send_dispatch, 0)

    def gather_copy(way, hop, d):
        step_back = hop - 1 if way else shards - hop + 1
        block = ring_map((place + step_back) % shards, shards)
        part = tokens.at[block, d, pl.ds(way * half, half)]
        return remote(
            part,
            part,
            gather_send.at[way, hop, d],
            gather_recv.at[way, hop, d],
            (me_s, before if way else after),
        )

    def sum_block(way, hop):
        if way:
            return ring_map((place + hop) % shards, shards)
        return ring_map((place + shards - hop) % shards, shards)

    def sum_copy(way, hop, d):
        source = sums.at[way, hop - 1, d]
        return remote(
            source,
            sums.at[way, hop, d],
            sum_send.at[way, hop, d],
            sum_recv.at[way, hop, d],
            (me_s, before if way else after),
        )

    def done_copy(d):
        return remote(
            done_out.at[d // sources, pl.ds((d % sources) * capacity, capacity)],
            done_in.at[d],
            done_send.at[d],
            done_recv.at[d],
            ((me_s + experts - d) % experts, me_t),
        )

    def expert(d):
        gate = jnp.zeros((2 * half, gate_v.shape[1]), jnp.float32)
        up = jnp.zeros((2 * half, gate_v.shape[1]), jnp.float32)
        for j in range(shards):
            rows = pl.ds(j * width, width)
            piece = tokens[j, d]
            gate += jnp.dot(piece, gate_v[rows, :], preferred_element_type=jnp.float32)
            up += jnp.dot(piece, up_v[rows, :], preferred_element_type=jnp.float32)
        clamped = jnp.minimum(gate, CLAMP_LIMIT)
        act = (
            (jnp.clip(up, -CLAMP_LIMIT, CLAMP_LIMIT) + 1.0)
            * clamped
            * jax.nn.sigmoid(SIGMOID_SCALE * clamped)
        ).astype(jnp.bfloat16)
        for j in range(shards):
            partial[j, d] = jnp.dot(
                act, down_v[:, j * width : (j + 1) * width], preferred_element_type=jnp.float32
            ).astype(jnp.bfloat16)

    last = shards - 1

    def step(i, c):
        @pl.when(i < groups)
        def _():
            def arrive(d, c):
                @pl.when(d > 0)
                def _():
                    dispatch_copy(d).wait_recv()

                return c

            lax.fori_loop(i * sources, (i + 1) * sources, arrive, 0)

            for way in range(2):
                gather_copy(way, 1, i).start()

        def gather_hop(hop, c):
            d = i - hop + 1

            @pl.when(jnp.logical_and(d >= 0, d < groups))
            def _():
                for way in range(2):
                    gather_copy(way, hop - 1, d).wait_recv()
                    gather_copy(way, hop, d).start()

            return c

        lax.fori_loop(2, shards, gather_hop, 0)

        def sum_hop(hop, c):
            d = i - last - hop + 1

            @pl.when(jnp.logical_and(d >= 0, d < groups))
            def _():
                for way in range(2):
                    sum_copy(way, hop - 1, d).wait_recv()
                    sums[way, hop - 1, d] = (
                        sums[way, hop - 1, d].astype(jnp.float32)
                        + partial[sum_block(way, hop), d, way * half : (way + 1) * half].astype(
                            jnp.float32
                        )
                    ).astype(jnp.bfloat16)
                    sum_copy(way, hop, d).start()

            return c

        lax.fori_loop(2, shards, sum_hop, 0)
        finished = i - 2 * last

        @pl.when(finished >= 0)
        def _():
            for way in range(2):
                sum_copy(way, last, finished).wait_recv()
                done_out[finished, way * half : (way + 1) * half] = (
                    sums[way, last, finished].astype(jnp.float32)
                    + partial[me_t, finished, way * half : (way + 1) * half].astype(jnp.float32)
                ).astype(jnp.bfloat16)

            def leave(d, c):
                @pl.when(d > 0)
                def _():
                    done_copy(d).start()

                return c

            lax.fori_loop(finished * sources, (finished + 1) * sources, leave, 0)

        ready = i - last

        @pl.when(jnp.logical_and(ready >= 0, ready < groups))
        def _():
            for way in range(2):
                gather_copy(way, last, ready).wait_recv()

            @pl.when(ready == 0)
            def _():
                for load in loads:
                    load.wait()

            expert(ready)
            for way in range(2):
                sums[way, 0, ready] = partial[
                    sum_block(way, 1), ready, way * half : (way + 1) * half
                ]
                sum_copy(way, 1, ready).start()

        return c

    lax.fori_loop(0, groups + 2 * last, step, 0)

    def combine(d, rows):
        weights = jnp.where(slots == rank_ref[d], weight_ref[d], 0.0)
        high = weights.astype(jnp.bfloat16)
        low = (weights - high.astype(jnp.float32)).astype(jnp.bfloat16)
        over_slots = (((0,), (0,)), ((), ()))
        return lax.dot_general(
            high, rows, over_slots, preferred_element_type=jnp.float32
        ) + lax.dot_general(low, rows, over_slots, preferred_element_type=jnp.float32)

    hidden[...] += combine(0, done_out[0, :capacity])

    def take_done(d, c):
        done_copy(d).wait_recv()
        hidden[...] += combine(d, done_in[d])
        return c

    lax.fori_loop(1, experts, take_done, 0)
    out_ref[...] = hidden[...].astype(jnp.bfloat16)

    def finish_tp(d, c):
        share_copy(d).wait_send()
        square_copy(d).wait_send()
        return c

    lax.fori_loop(1, shards, finish_tp, 0)

    def finish_sp(d, c):
        dispatch_copy(d).wait_send()
        done_copy(d).wait_send()
        return c

    lax.fori_loop(1, experts, finish_sp, 0)

    def finish_chunk(d, c):
        def finish_hop(hop, c):
            for way in range(2):
                gather_copy(way, hop, d).wait_send()
                sum_copy(way, hop, d).wait_send()
            return c

        return lax.fori_loop(1, shards, finish_hop, c)

    lax.fori_loop(0, groups, finish_chunk, 0)


def tail_call(*operands):
    *arrays, capacity = operands
    shards, experts = lax.axis_size("tp"), lax.axis_size("sp")
    length, width = arrays[4].shape
    gate, up, down = arrays[8:]
    sources = max(1, min(experts, 128 // capacity))
    groups = experts // sources
    rows = sources * capacity
    bf16, f32 = jnp.bfloat16, jnp.float32
    vmem = pl.BlockSpec(memory_space=pltpu.VMEM)
    dma = pltpu.SemaphoreType.DMA
    return pl.pallas_call(
        functools.partial(tail_kernel, shards, experts),
        out_shape=jax.ShapeDtypeStruct((length, width), bf16),
        in_specs=[vmem] * 8 + [pl.BlockSpec(memory_space=pl.ANY)] * 3,
        out_specs=vmem,
        scratch_shapes=[
            pltpu.VMEM(gate.shape, bf16),
            pltpu.VMEM(up.shape, bf16),
            pltpu.VMEM(down.shape, bf16),
            pltpu.VMEM((shards, length, width), bf16),
            pltpu.VMEM((shards, length, width), bf16),
            pltpu.VMEM((8, length), f32),
            pltpu.VMEM((shards, 8, length), f32),
            pltpu.VMEM((length, width), f32),
            pltpu.VMEM((length, width), bf16),
            pltpu.VMEM((experts, capacity, width), bf16),
            pltpu.VMEM((shards, groups, rows, width), bf16),
            pltpu.VMEM((shards, groups, rows, width), bf16),
            pltpu.VMEM((2, shards, groups, rows // 2, width), bf16),
            pltpu.VMEM((groups, rows, width), bf16),
            pltpu.VMEM((experts, capacity, width), bf16),
            dma((3,)),
            dma((shards,)),
            dma((shards,)),
            dma((shards,)),
            dma((shards,)),
            dma((experts,)),
            dma((experts,)),
            dma((2, shards, groups)),
            dma((2, shards, groups)),
            dma((2, shards, groups)),
            dma((2, shards, groups)),
            dma((experts,)),
            dma((experts,)),
        ],
        compiler_params=pltpu.CompilerParams(
            collective_id=0, has_side_effects=True, vmem_limit_bytes=56 * 1024 * 1024
        ),
    )(*arrays)


def local(
    resid,
    narrow_head_input,
    wide_head_input,
    key_group_input,
    query_group_input,
    narrow_output_gate,
    wide_output_gate,
    step_input_rows,
    head_decay_logarithm,
    position_log_decay,
    direct_input_weight,
    narrow_conv_taps,
    wide_conv_taps,
    key_conv_taps,
    query_conv_taps,
    narrow_norm_gain,
    wide_norm_gain,
    narrow_output_rows,
    wide_output_rows,
    feedforward_norm_gain,
    routes,
    routing_weight_values,
    expert_gate_matrix,
    expert_up_matrix,
    expert_down_matrix,
):
    length = resid.shape[0]
    head_count = narrow_head_input.shape[1] // NARROW_HEAD_DIM
    rim_len = narrow_conv_taps.shape[0] - 1
    rim_rows = passed_along(
        (
            narrow_head_input[length - rim_len :],
            wide_head_input[length - rim_len :],
            key_group_input[length - rim_len :],
            query_group_input[length - rim_len :],
        ),
        "sp",
        1,
    )
    narrow_head_mix = conv_with_rim(narrow_head_input, rim_rows[0], narrow_conv_taps).reshape(
        length, head_count, NARROW_HEAD_DIM
    )
    wide_head_mix = conv_with_rim(wide_head_input, rim_rows[1], wide_conv_taps).reshape(
        length, head_count, WIDE_HEAD_DIM
    )
    first_head = lax.axis_index("tp") * head_count
    key_head_rows = pick_groups(
        conv_with_rim(key_group_input, rim_rows[2], key_conv_taps), first_head, head_count
    )
    query_head_rows = pick_groups(
        conv_with_rim(query_group_input, rim_rows[3], query_conv_taps), first_head, head_count
    )
    step_length_values = jax.nn.softplus(step_input_rows.astype(jnp.float32))
    narrow_parts = head_pieces_list(
        narrow_head_mix,
        step_length_values[:, 0],
        head_decay_logarithm[0],
        position_log_decay[:, 0],
        key_head_rows,
        query_head_rows,
    )
    wide_parts = head_pieces_list(
        wide_head_mix,
        step_length_values[:, 1],
        head_decay_logarithm[1],
        position_log_decay[:, 1],
        key_head_rows,
        query_head_rows,
    )
    summary = (narrow_parts[3], wide_parts[3], narrow_parts[2], wide_parts[2])
    carried = entering_2(
        summary,
        "sp",
        chain_combine,
        (
            jnp.zeros_like(summary[0]),
            jnp.zeros_like(summary[1]),
            jnp.zeros_like(summary[2]),
            jnp.zeros_like(summary[3]),
        ),
    )
    narrow_carry, wide_carry = (carried[2], carried[3])
    narrow_head_output = group_out(
        finish_group(narrow_parts, narrow_carry),
        narrow_head_mix,
        direct_input_weight[0],
        narrow_output_gate,
        narrow_norm_gain,
    )
    wide_head_output = group_out(
        finish_group(wide_parts, wide_carry),
        wide_head_mix,
        direct_input_weight[1],
        wide_output_gate,
        wide_norm_gain,
    )
    experts = lax.axis_size("sp")
    shards = lax.axis_size("tp")
    picks = routes.shape[1]
    capacity = 4 * length * picks // (3 * experts)
    width = resid.shape[1] // shards
    tp_index = lax.axis_index("tp")
    expert_order = (lax.axis_index("sp") + jnp.arange(experts, dtype=jnp.int32)) % experts
    hits = routes[None] == expert_order[:, None, None]
    member = jnp.any(hits, axis=2)
    weight_rows = jnp.sum(jnp.where(hits, routing_weight_values[None], 0.0), axis=2)
    earlier = (jnp.arange(length)[:, None] < jnp.arange(length)[None, :]).astype(jnp.bfloat16)
    ranks = jnp.dot(
        member.astype(jnp.bfloat16), earlier, preferred_element_type=jnp.float32
    ).astype(jnp.int32)
    rank_rows = jnp.where(member, ranks, -1)
    resid_own = lax.dynamic_slice_in_dim(resid, tp_index * width, width, 1)
    gain_own = lax.dynamic_slice_in_dim(feedforward_norm_gain, tp_index * width, width, 0)
    return tail_call(
        narrow_head_output,
        wide_head_output,
        narrow_output_rows,
        wide_output_rows,
        resid_own,
        gain_own[None, :],
        rank_rows[:, None, :],
        weight_rows[:, None, :],
        expert_gate_matrix[0],
        expert_up_matrix[0],
        expert_down_matrix[0],
        capacity,
    )


def solution(mesh):
    return jax.shard_map(
        local,
        mesh=mesh,
        in_specs=(
            P("sp", None),
            P("sp", "tp"),
            P("sp", "tp"),
            P("sp", None),
            P("sp", None),
            P("sp", "tp"),
            P("sp", "tp"),
            P("sp", None, "tp"),
            P(None, "tp"),
            P("sp", None, "tp"),
            P(None, "tp"),
            P(None, "tp"),
            P(None, "tp"),
            P(),
            P(),
            P("tp"),
            P("tp"),
            P("tp", None),
            P("tp", None),
            P(),
            P("sp", None),
            P("sp", None),
            P("sp", None, "tp"),
            P("sp", None, "tp"),
            P("sp", "tp", None),
        ),
        out_specs=P("sp", "tp"),
        check_vma=False,
    )
```

```python
import functools

import jax
import jax.numpy as jnp
from jax import lax
from jax.experimental import pallas as pl
from jax.experimental.pallas import tpu as pltpu
from jax.sharding import PartitionSpec as P

HEADS = 16
NARROW_HEAD_DIM = 64
WIDE_HEAD_DIM = 128
GROUPS = 4
BLOCK = 128


NORM_EPS = 1e-06
CLAMP_LIMIT = 7.0
SIGMOID_SCALE = 1.702
FULL_PRECISION = lax.Precision.HIGHEST


def passed_along(block, axis, distance):
    devices = range(lax.axis_size(axis))
    route = [(i - distance, i) for i in devices if i - distance in devices]
    return lax.ppermute(block, axis, route)


def entering(narrow_parts, wide_parts, axis):
    place = lax.axis_index(axis)
    narrow_states, wide_states = narrow_parts[2], wide_parts[2]
    heads, state_size, narrow_size = narrow_states.shape
    totals = jnp.stack([narrow_parts[3], wide_parts[3]], axis=1)
    total_rows = jnp.broadcast_to(
        jnp.repeat(totals, 4, axis=1)[:, :, None], (heads, 8, narrow_size)
    )
    narrow_packed = jnp.concatenate([narrow_states, total_rows], axis=1).astype(jnp.bfloat16)
    narrow_all, wide_all = lax.all_gather((narrow_packed, wide_states.astype(jnp.bfloat16)), axis)
    count = narrow_all.shape[0]
    earlier = jnp.arange(count) < place
    between = jnp.logical_and(
        jnp.arange(count)[:, None] < jnp.arange(count)[None, :], earlier[None, :]
    )

    def carry(states, row):
        decay = narrow_all[:, :, state_size + row, 0].astype(jnp.float32)
        gap = jnp.sum(jnp.where(between[:, :, None], decay[None], 0.0), axis=1)
        factor = jnp.where(earlier[:, None], jnp.exp(gap), 0.0)
        return jnp.sum(factor[:, :, None, None] * states.astype(jnp.float32), axis=0)

    return carry(narrow_all[:, :, :state_size], 0), carry(wide_all, 4)


def conv_with_rim(values, rim_rows, weight):
    length = values.shape[0]
    padded = jnp.concatenate([rim_rows, values], axis=0).astype(jnp.float32)
    accumulated = jnp.zeros((length, values.shape[1]), jnp.float32)
    for tap_index in range(weight.shape[0]):
        accumulated = accumulated + weight[tap_index] * padded[tap_index : tap_index + length]
    return jax.nn.silu(accumulated)


def local_head(values, step_logarithm, key_head_rows, query_head_rows, block_len):
    block_count = values.shape[0] // block_len
    values = values.reshape(block_count, block_len, -1)
    step_logarithm = step_logarithm.reshape(block_count, block_len)
    key_head_rows = key_head_rows.reshape(block_count, block_len, -1)
    query_head_rows = query_head_rows.reshape(block_count, block_len, -1)
    cum_decay = jnp.cumsum(step_logarithm, axis=1)
    causal_mask = jnp.arange(block_len)[:, None] >= jnp.arange(block_len)[None, :]
    decay_gaps = jnp.where(causal_mask[None], cum_decay[:, :, None] - cum_decay[:, None, :], -1e30)
    scores = jnp.einsum(
        "bln,bsn->bls", query_head_rows, key_head_rows, precision=FULL_PRECISION
    ) * jnp.exp(decay_gaps)
    inside = jnp.einsum("bls,bsp->blp", scores, values, precision=FULL_PRECISION)
    tail_decay = jnp.exp(cum_decay[:, -1:] - cum_decay)
    states = jnp.einsum(
        "bln,blp->bnp", key_head_rows * tail_decay[..., None], values, precision=FULL_PRECISION
    )
    totals = cum_decay[:, -1]

    def walk(running, member):
        return (jnp.exp(member[1]) * running + member[0], running)

    closing, entering = lax.scan(walk, jnp.zeros(states.shape[1:], jnp.float32), (states, totals))
    before = jnp.cumsum(totals) - totals
    return (inside, entering, closing, jnp.sum(totals), before, cum_decay, query_head_rows)


def finish_head(inside, entering, before, cum_decay, query_blocks, carried):
    starting = entering + jnp.exp(before)[:, None, None] * carried[None]
    readout = jnp.einsum(
        "bln,bnp->blp",
        query_blocks * jnp.exp(cum_decay)[..., None],
        starting,
        precision=FULL_PRECISION,
    )
    return (inside + readout).reshape(-1, inside.shape[-1])


def group_out(scanned, mixed_input_rows, direct_input_term, gate_input_rows, norm_gain_vector):
    length, head_count, head_dimension = mixed_input_rows.shape
    gated = jax.nn.silu(gate_input_rows.astype(jnp.float32)).reshape(
        length, head_count, head_dimension
    )
    result = (scanned + direct_input_term[None, :, None] * mixed_input_rows) * gated
    result = result * lax.rsqrt(jnp.mean(result * result, axis=-1, keepdims=True) + NORM_EPS)
    return (result.reshape(length, head_count * head_dimension) * norm_gain_vector).astype(
        jnp.bfloat16
    )


def head_pieces_list(
    mixed_input_rows,
    step_length_values,
    decay_vector,
    position_decay_rows,
    key_head_rows,
    query_head_rows,
):
    step_logarithm = -jnp.exp(decay_vector)[None, :] * step_length_values + position_decay_rows
    values = mixed_input_rows * step_length_values[..., None]
    walker = functools.partial(local_head, block_len=BLOCK)
    return jax.vmap(walker, in_axes=(1, 1, None, None))(
        values, step_logarithm, key_head_rows, query_head_rows
    )


def finish_group(parts, carried_states):
    return jax.vmap(finish_head, in_axes=(0, 0, 0, 0, 0, 0), out_axes=1)(
        parts[0], parts[1], parts[4], parts[5], parts[6], carried_states
    )


def ring_map(index, count):
    side = int(round(count**0.5))
    if side * side != count:
        return index
    row = index // side
    column = index % side
    return row * side + column + (row % 2) * (side - 1 - 2 * column)


def tail_kernel(
    shards,
    experts,
    narrow_ref,
    wide_ref,
    narrow_rows_ref,
    wide_rows_ref,
    resid_ref,
    gain_ref,
    rank_ref,
    weight_ref,
    gate_hbm,
    up_hbm,
    down_hbm,
    out_ref,
    gate_v,
    up_v,
    down_v,
    share_out,
    share_in,
    square_out,
    square_in,
    hidden,
    normed,
    dispatch_out,
    tokens,
    partial,
    sums,
    done_out,
    done_in,
    load_sem,
    share_send,
    share_recv,
    square_send,
    square_recv,
    dispatch_send,
    dispatch_recv,
    gather_send,
    gather_recv,
    sum_send,
    sum_recv,
    done_send,
    done_recv,
):
    me_s = lax.axis_index("sp")
    me_t = lax.axis_index("tp")
    length, width = resid_ref.shape
    capacity = done_in.shape[1]
    groups = tokens.shape[1]
    sources = experts // groups
    half = tokens.shape[2] // 2
    place = ring_map(me_t, shards)
    after = ring_map((place + 1) % shards, shards)
    before = ring_map((place + shards - 1) % shards, shards)

    def remote(src, dst, send, recv, where):
        return pltpu.make_async_remote_copy(
            src_ref=src,
            dst_ref=dst,
            send_sem=send,
            recv_sem=recv,
            device_id=where,
            device_id_type=pl.DeviceIdType.MESH,
        )

    loads = [
        pltpu.make_async_copy(h, v, load_sem.at[i])
        for i, (h, v) in enumerate(((gate_hbm, gate_v), (up_hbm, up_v), (down_hbm, down_v)))
    ]
    for load in loads:
        load.start()

    barrier = pltpu.get_barrier_semaphore()

    def greet_tp(d, c):
        pl.semaphore_signal(
            barrier,
            inc=1,
            device_id=(me_s, (me_t + d) % shards),
            device_id_type=pl.DeviceIdType.MESH,
        )
        return c

    def greet_sp(d, c):
        pl.semaphore_signal(
            barrier,
            inc=1,
            device_id=((me_s + d) % experts, me_t),
            device_id_type=pl.DeviceIdType.MESH,
        )
        return c

    lax.fori_loop(1, shards, greet_tp, 0)
    lax.fori_loop(1, experts, greet_sp, 0)
    pl.semaphore_wait(barrier, shards + experts - 2)

    def project(block):
        columns = pl.ds(pl.multiple_of(block * width, 128), width)
        return (
            jnp.dot(
                narrow_ref[...], narrow_rows_ref[:, columns], preferred_element_type=jnp.float32
            )
            + jnp.dot(wide_ref[...], wide_rows_ref[:, columns], preferred_element_type=jnp.float32)
        ).astype(jnp.bfloat16)

    def share_copy(d):
        return remote(
            share_out.at[d],
            share_in.at[d],
            share_send.at[d],
            share_recv.at[d],
            (me_s, (me_t + d) % shards),
        )

    def send_share(d, c):
        share_out[d] = project((me_t + d) % shards)
        share_copy(d).start()
        return c

    lax.fori_loop(1, shards, send_share, 0)
    hidden[...] = resid_ref[...].astype(jnp.float32) + project(me_t).astype(jnp.float32)

    def take_share(d, c):
        share_copy(d).wait_recv()
        hidden[...] += share_in[d].astype(jnp.float32)
        return c

    lax.fori_loop(1, shards, take_share, 0)
    state = hidden[...]
    own_square = jnp.sum(state * state, axis=1, keepdims=True)
    square_rows = jnp.transpose(jnp.broadcast_to(own_square, (length, 128)))
    square_out[...] = square_rows[:8]

    def square_copy(d):
        return remote(
            square_out,
            square_in.at[d],
            square_send.at[d],
            square_recv.at[d],
            (me_s, (me_t + d) % shards),
        )

    def send_square(d, c):
        square_copy(d).start()
        return c

    lax.fori_loop(1, shards, send_square, 0)

    def take_square(d, total):
        square_copy(d).wait_recv()
        return total + square_in[d]

    total = lax.fori_loop(1, shards, take_square, square_rows[:8])
    scale_row = lax.rsqrt(total[:1] / (shards * width) + NORM_EPS)
    scale = jnp.transpose(jnp.broadcast_to(scale_row, (128, length)))[:, :1]
    normed[...] = (hidden[...] * scale * gain_ref[...]).astype(jnp.bfloat16)

    slots = lax.broadcasted_iota(jnp.int32, (capacity, length), 0)

    def pick(d):
        chooser = jnp.where(slots == rank_ref[d], 1.0, 0.0).astype(jnp.bfloat16)
        return jnp.dot(chooser, normed[...], preferred_element_type=jnp.float32).astype(
            jnp.bfloat16
        )

    def dispatch_copy(d):
        return remote(
            dispatch_out.at[d],
            tokens.at[me_t, d // sources, pl.ds((d % sources) * capacity, capacity)],
            dispatch_send.at[d],
            dispatch_recv.at[d],
            ((me_s + d) % experts, me_t),
        )

    def send_dispatch(d, c):
        dispatch_out[d] = pick(d)
        dispatch_copy(d).start()
        return c

    tokens[me_t, 0, :capacity] = pick(0)
    lax.fori_loop(1, experts, send_dispatch, 0)

    def gather_copy(way, hop, d):
        step_back = hop - 1 if way else shards - hop + 1
        block = ring_map((place + step_back) % shards, shards)
        part = tokens.at[block, d, pl.ds(way * half, half)]
        return remote(
            part,
            part,
            gather_send.at[way, hop, d],
            gather_recv.at[way, hop, d],
            (me_s, before if way else after),
        )

    def sum_block(way, hop):
        if way:
            return ring_map((place + hop) % shards, shards)
        return ring_map((place + shards - hop) % shards, shards)

    def sum_copy(way, hop, d):
        source = sums.at[way, hop - 1, d]
        return remote(
            source,
            sums.at[way, hop, d],
            sum_send.at[way, hop, d],
            sum_recv.at[way, hop, d],
            (me_s, before if way else after),
        )

    def done_copy(d):
        return remote(
            done_out.at[d // sources, pl.ds((d % sources) * capacity, capacity)],
            done_in.at[d],
            done_send.at[d],
            done_recv.at[d],
            ((me_s + experts - d) % experts, me_t),
        )

    def expert(d):
        gate = jnp.zeros((2 * half, gate_v.shape[1]), jnp.float32)
        up = jnp.zeros((2 * half, gate_v.shape[1]), jnp.float32)
        for j in range(shards):
            rows = pl.ds(j * width, width)
            piece = tokens[j, d]
            gate += jnp.dot(piece, gate_v[rows, :], preferred_element_type=jnp.float32)
            up += jnp.dot(piece, up_v[rows, :], preferred_element_type=jnp.float32)
        clamped = jnp.minimum(gate, CLAMP_LIMIT)
        act = (
            (jnp.clip(up, -CLAMP_LIMIT, CLAMP_LIMIT) + 1.0)
            * clamped
            * jax.nn.sigmoid(SIGMOID_SCALE * clamped)
        ).astype(jnp.bfloat16)
        for j in range(shards):
            partial[j, d] = jnp.dot(
                act, down_v[:, j * width : (j + 1) * width], preferred_element_type=jnp.float32
            ).astype(jnp.bfloat16)

    last = shards - 1

    def step(i, c):
        @pl.when(i < groups)
        def _():
            def arrive(d, c):
                @pl.when(d > 0)
                def _():
                    dispatch_copy(d).wait_recv()

                return c

            lax.fori_loop(i * sources, (i + 1) * sources, arrive, 0)

            for way in range(2):
                gather_copy(way, 1, i).start()

        def gather_hop(hop, c):
            d = i - hop + 1

            @pl.when(jnp.logical_and(d >= 0, d < groups))
            def _():
                for way in range(2):
                    gather_copy(way, hop - 1, d).wait_recv()
                    gather_copy(way, hop, d).start()

            return c

        lax.fori_loop(2, shards, gather_hop, 0)

        def sum_hop(hop, c):
            d = i - last - hop + 1

            @pl.when(jnp.logical_and(d >= 0, d < groups))
            def _():
                for way in range(2):
                    sum_copy(way, hop - 1, d).wait_recv()
                    sums[way, hop - 1, d] = (
                        sums[way, hop - 1, d].astype(jnp.float32)
                        + partial[sum_block(way, hop), d, way * half : (way + 1) * half].astype(
                            jnp.float32
                        )
                    ).astype(jnp.bfloat16)
                    sum_copy(way, hop, d).start()

            return c

        lax.fori_loop(2, shards, sum_hop, 0)
        finished = i - 2 * last

        @pl.when(finished >= 0)
        def _():
            for way in range(2):
                sum_copy(way, last, finished).wait_recv()
                done_out[finished, way * half : (way + 1) * half] = (
                    sums[way, last, finished].astype(jnp.float32)
                    + partial[me_t, finished, way * half : (way + 1) * half].astype(jnp.float32)
                ).astype(jnp.bfloat16)

            def leave(d, c):
                @pl.when(d > 0)
                def _():
                    done_copy(d).start()

                return c

            lax.fori_loop(finished * sources, (finished + 1) * sources, leave, 0)

        ready = i - last

        @pl.when(jnp.logical_and(ready >= 0, ready < groups))
        def _():
            for way in range(2):
                gather_copy(way, last, ready).wait_recv()

            @pl.when(ready == 0)
            def _():
                for load in loads:
                    load.wait()

            expert(ready)
            for way in range(2):
                sums[way, 0, ready] = partial[
                    sum_block(way, 1), ready, way * half : (way + 1) * half
                ]
                sum_copy(way, 1, ready).start()

        return c

    lax.fori_loop(0, groups + 2 * last, step, 0)

    def combine(d, rows):
        weights = jnp.where(slots == rank_ref[d], weight_ref[d], 0.0)
        high = weights.astype(jnp.bfloat16)
        low = (weights - high.astype(jnp.float32)).astype(jnp.bfloat16)
        over_slots = (((0,), (0,)), ((), ()))
        return lax.dot_general(
            high, rows, over_slots, preferred_element_type=jnp.float32
        ) + lax.dot_general(low, rows, over_slots, preferred_element_type=jnp.float32)

    hidden[...] += combine(0, done_out[0, :capacity])

    def take_done(d, c):
        done_copy(d).wait_recv()
        hidden[...] += combine(d, done_in[d])
        return c

    lax.fori_loop(1, experts, take_done, 0)
    out_ref[...] = hidden[...].astype(jnp.bfloat16)

    def finish_tp(d, c):
        share_copy(d).wait_send()
        square_copy(d).wait_send()
        return c

    lax.fori_loop(1, shards, finish_tp, 0)

    def finish_sp(d, c):
        dispatch_copy(d).wait_send()
        done_copy(d).wait_send()
        return c

    lax.fori_loop(1, experts, finish_sp, 0)

    def finish_chunk(d, c):
        def finish_hop(hop, c):
            for way in range(2):
                gather_copy(way, hop, d).wait_send()
                sum_copy(way, hop, d).wait_send()
            return c

        return lax.fori_loop(1, shards, finish_hop, c)

    lax.fori_loop(0, groups, finish_chunk, 0)


def tail_call(*operands):
    *arrays, capacity = operands
    shards, experts = lax.axis_size("tp"), lax.axis_size("sp")
    length, width = arrays[4].shape
    gate, up, down = arrays[8:]
    sources = max(1, min(experts, 128 // capacity))
    groups = experts // sources
    rows = sources * capacity
    bf16, f32 = jnp.bfloat16, jnp.float32
    vmem = pl.BlockSpec(memory_space=pltpu.VMEM)
    dma = pltpu.SemaphoreType.DMA
    return pl.pallas_call(
        functools.partial(tail_kernel, shards, experts),
        out_shape=jax.ShapeDtypeStruct((length, width), bf16),
        in_specs=[vmem] * 8 + [pl.BlockSpec(memory_space=pl.ANY)] * 3,
        out_specs=vmem,
        scratch_shapes=[
            pltpu.VMEM(gate.shape, bf16),
            pltpu.VMEM(up.shape, bf16),
            pltpu.VMEM(down.shape, bf16),
            pltpu.VMEM((shards, length, width), bf16),
            pltpu.VMEM((shards, length, width), bf16),
            pltpu.VMEM((8, length), f32),
            pltpu.VMEM((shards, 8, length), f32),
            pltpu.VMEM((length, width), f32),
            pltpu.VMEM((length, width), bf16),
            pltpu.VMEM((experts, capacity, width), bf16),
            pltpu.VMEM((shards, groups, rows, width), bf16),
            pltpu.VMEM((shards, groups, rows, width), bf16),
            pltpu.VMEM((2, shards, groups, rows // 2, width), bf16),
            pltpu.VMEM((groups, rows, width), bf16),
            pltpu.VMEM((experts, capacity, width), bf16),
            dma((3,)),
            dma((shards,)),
            dma((shards,)),
            dma((shards,)),
            dma((shards,)),
            dma((experts,)),
            dma((experts,)),
            dma((2, shards, groups)),
            dma((2, shards, groups)),
            dma((2, shards, groups)),
            dma((2, shards, groups)),
            dma((experts,)),
            dma((experts,)),
        ],
        compiler_params=pltpu.CompilerParams(
            collective_id=0, has_side_effects=True, vmem_limit_bytes=56 * 1024 * 1024
        ),
    )(*arrays)


def local(
    resid,
    narrow_head_input,
    wide_head_input,
    key_group_input,
    query_group_input,
    narrow_output_gate,
    wide_output_gate,
    step_input_rows,
    head_decay_logarithm,
    position_log_decay,
    direct_input_weight,
    narrow_conv_taps,
    wide_conv_taps,
    key_conv_taps,
    query_conv_taps,
    narrow_norm_gain,
    wide_norm_gain,
    narrow_output_rows,
    wide_output_rows,
    feedforward_norm_gain,
    routes,
    routing_weight_values,
    expert_gate_matrix,
    expert_up_matrix,
    expert_down_matrix,
):
    length = resid.shape[0]
    head_count = narrow_head_input.shape[1] // NARROW_HEAD_DIM
    rim_len = narrow_conv_taps.shape[0] - 1
    first_head = lax.axis_index("tp") * head_count
    state_size = key_group_input.shape[1] // GROUPS
    group_column = first_head // (HEADS // GROUPS) * state_size

    def own_group(table):
        return lax.dynamic_slice_in_dim(table, group_column, state_size, 1)

    streams = (
        narrow_head_input,
        wide_head_input,
        own_group(key_group_input),
        own_group(query_group_input),
    )
    rims = passed_along(
        jnp.concatenate([stream[length - rim_len :] for stream in streams], axis=1), "sp", 1
    )
    edges = [0]
    for stream in streams:
        edges.append(edges[-1] + stream.shape[1])
    rim_rows = [rims[:, low:high] for low, high in zip(edges[:-1], edges[1:])]
    narrow_head_mix = conv_with_rim(narrow_head_input, rim_rows[0], narrow_conv_taps).reshape(
        length, head_count, NARROW_HEAD_DIM
    )
    wide_head_mix = conv_with_rim(wide_head_input, rim_rows[1], wide_conv_taps).reshape(
        length, head_count, WIDE_HEAD_DIM
    )
    key_head_rows = conv_with_rim(streams[2], rim_rows[2], own_group(key_conv_taps))
    query_head_rows = conv_with_rim(streams[3], rim_rows[3], own_group(query_conv_taps))
    step_length_values = jax.nn.softplus(step_input_rows.astype(jnp.float32))
    narrow_parts = head_pieces_list(
        narrow_head_mix,
        step_length_values[:, 0],
        head_decay_logarithm[0],
        position_log_decay[:, 0],
        key_head_rows,
        query_head_rows,
    )
    wide_parts = head_pieces_list(
        wide_head_mix,
        step_length_values[:, 1],
        head_decay_logarithm[1],
        position_log_decay[:, 1],
        key_head_rows,
        query_head_rows,
    )
    narrow_carry, wide_carry = entering(narrow_parts, wide_parts, "sp")
    narrow_head_output = group_out(
        finish_group(narrow_parts, narrow_carry),
        narrow_head_mix,
        direct_input_weight[0],
        narrow_output_gate,
        narrow_norm_gain,
    )
    wide_head_output = group_out(
        finish_group(wide_parts, wide_carry),
        wide_head_mix,
        direct_input_weight[1],
        wide_output_gate,
        wide_norm_gain,
    )
    experts = lax.axis_size("sp")
    shards = lax.axis_size("tp")
    picks = routes.shape[1]
    capacity = 4 * length * picks // (3 * experts)
    width = resid.shape[1] // shards
    tp_index = lax.axis_index("tp")
    expert_order = (lax.axis_index("sp") + jnp.arange(experts, dtype=jnp.int32)) % experts
    hits = routes[None] == expert_order[:, None, None]
    member = jnp.any(hits, axis=2)
    weight_rows = jnp.sum(jnp.where(hits, routing_weight_values[None], 0.0), axis=2)
    earlier = (jnp.arange(length)[:, None] < jnp.arange(length)[None, :]).astype(jnp.bfloat16)
    ranks = jnp.dot(
        member.astype(jnp.bfloat16), earlier, preferred_element_type=jnp.float32
    ).astype(jnp.int32)
    rank_rows = jnp.where(member, ranks, -1)
    resid_own = lax.dynamic_slice_in_dim(resid, tp_index * width, width, 1)
    gain_own = lax.dynamic_slice_in_dim(feedforward_norm_gain, tp_index * width, width, 0)
    return tail_call(
        narrow_head_output,
        wide_head_output,
        narrow_output_rows,
        wide_output_rows,
        resid_own,
        gain_own[None, :],
        rank_rows[:, None, :],
        weight_rows[:, None, :],
        expert_gate_matrix[0],
        expert_up_matrix[0],
        expert_down_matrix[0],
        capacity,
    )


def solution(mesh):
    return jax.shard_map(
        local,
        mesh=mesh,
        in_specs=(
            P("sp", None),
            P("sp", "tp"),
            P("sp", "tp"),
            P("sp", None),
            P("sp", None),
            P("sp", "tp"),
            P("sp", "tp"),
            P("sp", None, "tp"),
            P(None, "tp"),
            P("sp", None, "tp"),
            P(None, "tp"),
            P(None, "tp"),
            P(None, "tp"),
            P(),
            P(),
            P("tp"),
            P("tp"),
            P("tp", None),
            P("tp", None),
            P(),
            P("sp", None),
            P("sp", None),
            P("sp", None, "tp"),
            P("sp", None, "tp"),
            P("sp", "tp", None),
        ),
        out_specs=P("sp", "tp"),
        check_vma=False,
    )
```
